32 devices in a mesh: sp: 16 (over z, y, x), dp: 2 (over core).
Axes of the slice: x: 2, y: 2, z: 4, core: 2. Of those that a mesh axis runs over, the one named last changes fastest.
Arguments:
- inputs: bfloat16 [2, 2048, 2048], P('dp', 'sp'), may hold values from -6 to 6
- w_key: bfloat16 [2048, 256], P('dp')
- w_value: bfloat16 [2048, 256], P('dp'), may hold values from -0.125 to 0.125
- queries: bfloat16 [2, 2048, 2048], P('dp', 'sp')
- cotangent: bfloat16 [2, 2048, 2048], P('dp', 'sp'), may hold values from -6 to 6
- cum_gate: float32 [2, 32, 2048], P('dp', 'sp'), as said below
Outputs:
- grad_input: bfloat16 [2, 2048, 2048], P('dp', 'sp')
- grad_queries: bfloat16 [2, 2048, 2048], P('dp', 'sp')
- grad_cum: float32 [2, 32, 2048], P('dp', 'sp')
- grad_w_key: float32 [2048, 256], P('dp')
- grad_w_value: float32 [2048, 256], P('dp')
The draws below stay inside these ranges and needn't reach their ends.
Inputs may be any that keep to these rules, and one draw needn't show every extreme that they name: Along each sequence cum_gate never rises, and it is at most zero.
All inputs are finite; a program needn't handle non-finite values.
Results may differ from the reference program's by a relative error of at most 0.023.
Values may be sent and summed in bfloat16 or wider, within the bound.
A program may use at most 128 MiB of HBM per device.

```python
import jax
import jax.numpy as jnp
from jax import lax

D = 2048
QUERY_HEADS_TOTAL = 32
HD = 64
KVH = 4
POS_DEV = 128
SEQUENCE_LENGTH = 2048
SEQUENCE_COUNT = 2


def shared_inputs(key):
    feature_key = jax.random.fold_in(key, 11)
    drawn = jnp.clip(jax.random.normal(feature_key, (SEQUENCE_COUNT, SEQUENCE_LENGTH, D), jnp.float32), -6.0, 6.0)
    return drawn


def shared_keyweight(key):
    drawn = jax.random.normal(jax.random.fold_in(key, 12), (D, KVH * HD), jnp.float32)
    return jnp.clip(drawn, -6.0, 6.0) * D ** (-0.5)


def draw_inputs(key, part):
    return shared_inputs(key).astype(jnp.bfloat16)


def draw_w_key(key, part):
    return shared_keyweight(key).astype(jnp.bfloat16)


def draw_queries(key, part):
    base_key = jax.random.fold_in(key, 13)
    drawn = jnp.clip(jax.random.normal(base_key, (SEQUENCE_COUNT, SEQUENCE_LENGTH, QUERY_HEADS_TOTAL * HD), jnp.float32), -6.0, 6.0)
    return drawn.astype(jnp.bfloat16)


def draw_cum_gate(key, part):
    gate_random_keys = jax.random.split(jax.random.fold_in(key, 31), 7)
    share = 0.5
    gradual_gate = jax.random.uniform(gate_random_keys[0], (1, QUERY_HEADS_TOTAL, 1), jnp.float32) < share
    total = jax.random.uniform(gate_random_keys[1], (SEQUENCE_COUNT, QUERY_HEADS_TOTAL, 1), jnp.float32, 0.3, 1.2)
    fast_span = jax.random.uniform(gate_random_keys[2], (SEQUENCE_COUNT, QUERY_HEADS_TOTAL, 1), jnp.float32, 30.0, 100.0)
    decay_rate = jnp.where(gradual_gate, total / SEQUENCE_LENGTH, 1.0 / fast_span)
    block_multiplier = jnp.exp(jax.random.uniform(gate_random_keys[3], (SEQUENCE_COUNT, QUERY_HEADS_TOTAL, SEQUENCE_LENGTH // POS_DEV), jnp.float32, -0.8, 0.8))
    block_multiplier = jnp.repeat(block_multiplier, POS_DEV, axis=2)
    coarse_gate = jax.random.uniform(gate_random_keys[4], (SEQUENCE_COUNT, QUERY_HEADS_TOTAL, SEQUENCE_LENGTH), jnp.float32, 0.5, 1.5)
    spike_position = jax.random.randint(gate_random_keys[5], (SEQUENCE_COUNT, QUERY_HEADS_TOTAL, 3), 0, SEQUENCE_LENGTH)
    spike_length = jnp.log(jax.random.uniform(gate_random_keys[6], (SEQUENCE_COUNT, QUERY_HEADS_TOTAL, 3), jnp.float32, 0.55, 0.8))
    spike_flags = jnp.arange(SEQUENCE_LENGTH)[None, None, None, :] == spike_position[:, :, :, None]
    spike_events = jnp.sum(jnp.where(spike_flags, spike_length[:, :, :, None], 0.0), axis=2)
    gate_logarithm = -decay_rate * block_multiplier * coarse_gate + jnp.where(gradual_gate, spike_events, 0.0)
    return jnp.cumsum(gate_logarithm, axis=2)


def steps_of(stream_key, extent, pieces, smallest, top_value):
    def one(axis_at, shards_of):
        heights = jax.random.uniform(jax.random.fold_in(jax.random.fold_in(stream_key, 6), axis_at), (shards_of,), jnp.float32, smallest / len(pieces), top_value / len(pieces))
        return jnp.repeat(jnp.exp(heights), extent[axis_at] // shards_of).reshape((-1,) + (1,) * (len(extent) - axis_at - 1))

    level = one(*pieces[0])
    for cut in pieces[1:]:
        level = level * one(*cut)
    return level


def centred(stream_key, dims, width, most, shards=(), held_as=jnp.bfloat16):
    values = width * jax.random.normal(stream_key, dims, jnp.float32)
    if shards:
        values = values * steps_of(stream_key, dims, shards, -0.22, 0.18)
    return jnp.clip(values, -most, most).astype(held_as)


def setup_inputs(seed: int = 0) -> dict:
    streams_of = jax.random.split(jax.random.key(seed), 7)
    return {
        "inputs": draw_inputs(jax.random.fold_in(streams_of[6], 71), 0),
        "w_key": draw_w_key(jax.random.fold_in(streams_of[6], 71), 0),
        "w_value": centred(streams_of[2], (D, KVH * HD), D ** -0.5, 0.125, ((0, 2),)),
        "queries": draw_queries(jax.random.fold_in(streams_of[6], 71), 0),
        "cotangent": centred(streams_of[4], (SEQUENCE_COUNT, SEQUENCE_LENGTH, QUERY_HEADS_TOTAL * HD), 1.0, 6.0, ((0, 2), (1, 16))),
        "cum_gate": draw_cum_gate(jax.random.fold_in(streams_of[6], 71), 0),
    }


def head_backward(item_parts):
    query_rows, key_rows, value_rows, grad_rows, cum_rows = item_parts
    seq_length = query_rows.shape[0]
    score_scale = HD ** -0.5
    scores = jnp.dot(query_rows, key_rows.T, preferred_element_type=jnp.float32) * score_scale
    scores = scores + cum_rows[:, None] - cum_rows[None, :]
    later = jnp.arange(seq_length)[None, :] > jnp.arange(seq_length)[:, None]
    scores = jnp.where(later, -jnp.inf, scores)
    row_max = jnp.max(scores, axis=1, keepdims=True)
    exp_scores = jnp.exp(scores - row_max)
    probs = exp_scores / jnp.sum(exp_scores, axis=1, keepdims=True)
    probs_low = probs.astype(jnp.bfloat16)
    outputs = jnp.dot(probs_low, value_rows, preferred_element_type=jnp.float32)
    row_dot = jnp.sum(grad_rows.astype(jnp.float32) * outputs, axis=1)
    grad_probs = jnp.dot(grad_rows, value_rows.T, preferred_element_type=jnp.float32)
    grad_scores = probs * (grad_probs - row_dot[:, None])
    grad_low = grad_scores.astype(jnp.bfloat16)
    grad_query = (jnp.dot(grad_low, key_rows, preferred_element_type=jnp.float32) * score_scale).astype(jnp.bfloat16)
    key_term = (jnp.dot(grad_low.T, query_rows, preferred_element_type=jnp.float32) * score_scale).astype(jnp.bfloat16)
    value_term = jnp.dot(probs_low.T, grad_rows, preferred_element_type=jnp.float32).astype(jnp.bfloat16)
    grad_cum = jnp.sum(grad_scores, axis=1) - jnp.sum(grad_scores, axis=0)
    return grad_query, key_term, value_term, grad_cum


def reference(inputs, w_key, w_value, queries, cotangent, cum_gate):
    seq_count, seq_length, feature_count = inputs.shape
    group_size = QUERY_HEADS_TOTAL // KVH
    flat_rows = inputs.reshape(seq_count * seq_length, feature_count)
    key_proj = jnp.dot(flat_rows, w_key, preferred_element_type=jnp.float32).astype(jnp.bfloat16)
    value_proj = jnp.dot(flat_rows, w_value, preferred_element_type=jnp.float32).astype(jnp.bfloat16)

    def spread(projected):
        split_heads = projected.reshape(seq_count, seq_length, KVH, HD)
        repeated = jnp.repeat(split_heads, group_size, axis=2)
        return repeated.transpose(0, 2, 1, 3).reshape(seq_count * QUERY_HEADS_TOTAL, seq_length, HD)

    def by_head(tensor):
        return tensor.reshape(seq_count, seq_length, QUERY_HEADS_TOTAL, HD).transpose(0, 2, 1, 3).reshape(seq_count * QUERY_HEADS_TOTAL, seq_length, HD)

    grad_query, key_term, value_term, grad_cum = lax.map(
        head_backward,
        (by_head(queries), spread(key_proj), spread(value_proj), by_head(cotangent),
         cum_gate.reshape(seq_count * QUERY_HEADS_TOTAL, seq_length)))

    def to_tokens(tensor):
        return tensor.reshape(seq_count, QUERY_HEADS_TOTAL, seq_length, HD).transpose(0, 2, 1, 3)

    grad_queries = to_tokens(grad_query).reshape(seq_count, seq_length, QUERY_HEADS_TOTAL * HD)

    def group_sum(tensor):
        grouped = to_tokens(tensor).reshape(seq_count * seq_length, KVH, group_size, HD)
        return jnp.sum(grouped.astype(jnp.float32), axis=2).astype(jnp.bfloat16).reshape(seq_count * seq_length, KVH * HD)

    grad_keys = group_sum(key_term)
    grad_values = group_sum(value_term)
    grad_input = (jnp.dot(grad_keys, w_key.T, preferred_element_type=jnp.float32)
                  + jnp.dot(grad_values, w_value.T, preferred_element_type=jnp.float32)).astype(jnp.bfloat16)
    grad_w_key = jnp.dot(flat_rows.T, grad_keys, preferred_element_type=jnp.float32)
    grad_w_value = jnp.dot(flat_rows.T, grad_values, preferred_element_type=jnp.float32)
    return (grad_input.reshape(seq_count, seq_length, feature_count), grad_queries,
            grad_cum.reshape(seq_count, QUERY_HEADS_TOTAL, seq_length), grad_w_key, grad_w_value)
```

```python
import functools

import jax
import jax.numpy as jnp
from jax import lax
from jax.experimental import pallas as pl
from jax.experimental.pallas import tpu as pltpu
from jax.sharding import PartitionSpec as P

HD = 64
LANES = 128
LOG2E = 1.4426950408889634
MESH = pl.DeviceIdType.MESH
VMEM = pl.BlockSpec(memory_space=pltpu.VMEM)
BF16 = jnp.bfloat16
F32 = jnp.float32


def dot_nn(a, b):
    return jnp.dot(a, b, preferred_element_type=F32)


def dot_nt(a, b):
    return lax.dot_general(a, b, (((1,), (1,)), ((), ())), preferred_element_type=F32)


def dot_tn(a, b):
    return lax.dot_general(a, b, (((0,), (0,)), ((), ())), preferred_element_type=F32)


def greet(n, m):
    me, mine = lax.axis_index("sp"), lax.axis_index("dp")
    barrier = pltpu.get_barrier_semaphore()

    @pl.loop(1, n)
    def _(k):
        pl.semaphore_signal(
            barrier, inc=1, device_id={"sp": lax.rem(me + k, n)}, device_id_type=MESH
        )

    @pl.loop(1, m)
    def _(k):
        pl.semaphore_signal(
            barrier, inc=1, device_id={"dp": lax.rem(mine + k, m)}, device_id_type=MESH
        )

    pl.semaphore_wait(barrier, n + m - 2)


def start_all(n, make):
    @pl.loop(1, n)
    def _(k):
        make(k).start()


def wait_all(n, make):
    @pl.loop(1, n)
    def _(k):
        make(k).wait()


def remote(src, dst, sems, k, device):
    return pltpu.make_async_remote_copy(
        src_ref=src,
        dst_ref=dst,
        send_sem=sems.at[0, k],
        recv_sem=sems.at[1, k],
        device_id=device,
        device_id_type=MESH,
    )


def column_block(ref, j, width):
    if len(ref.shape) == 3:
        return ref.at[j]
    return ref.at[:, pl.ds(pl.multiple_of(j * width, LANES), width)]


def row_block(ref, j, rows):
    return ref.at[pl.ds(pl.multiple_of(j * rows, 16), rows)]


def gather_kernel(
    n, m, width, kv_heads,
    q_ref, g_ref, x_ref, wk_ref, wv_ref,
    q_out, g_out, kv_out, w_out, x_out,
    kv_block, q_sems, g_sems, kv_sems, wk_sems, wv_sems, x_sems, own_sems,
):
    me, mine = lax.axis_index("sp"), lax.axis_index("dp")
    positions = x_ref.shape[0]
    rows, kv_width = wk_ref.shape
    greet(n, m)

    def target(k):
        return lax.rem(me + k, n)

    def peer(k):
        return lax.rem(mine + k, m)

    def wk_copy(k):
        dst = row_block(w_out, mine, rows).at[:, pl.ds(0, kv_width)]
        return remote(wk_ref, dst, wk_sems, k, {"dp": peer(k)})

    def wv_copy(k):
        dst = row_block(w_out, mine, rows).at[:, pl.ds(kv_width, kv_width)]
        return remote(wv_ref, dst, wv_sems, k, {"dp": peer(k)})

    def x_copy(k):
        return remote(
            column_block(x_ref, peer(k), rows), x_out.at[mine], x_sems, k, {"dp": peer(k)}
        )

    def q_copy(k):
        return remote(
            column_block(q_ref, target(k), width),
            row_block(q_out, me, positions), q_sems, k, {"sp": target(k)},
        )

    def g_copy(k):
        return remote(
            column_block(g_ref, target(k), width),
            row_block(g_out, me, positions), g_sems, k, {"sp": target(k)},
        )

    def kv_copy(k):
        group = (target(k) * kv_heads) // n
        return remote(
            column_block(kv_block, group, 2 * HD),
            row_block(kv_out, me, positions), kv_sems, k, {"sp": target(k)},
        )

    own = [
        pltpu.make_async_copy(
            wk_ref, row_block(w_out, mine, rows).at[:, pl.ds(0, kv_width)], own_sems.at[0]
        ),
        pltpu.make_async_copy(
            wv_ref, row_block(w_out, mine, rows).at[:, pl.ds(kv_width, kv_width)], own_sems.at[1]
        ),
        pltpu.make_async_copy(column_block(x_ref, mine, rows), x_out.at[mine], own_sems.at[2]),
        pltpu.make_async_copy(
            column_block(q_ref, me, width), row_block(q_out, me, positions), own_sems.at[3]
        ),
        pltpu.make_async_copy(
            column_block(g_ref, me, width), row_block(g_out, me, positions), own_sems.at[4]
        ),
    ]
    start_all(m, wk_copy)
    start_all(m, wv_copy)
    start_all(n, q_copy)
    start_all(n, g_copy)
    for copy in own:
        copy.start()
    wait_all(m, wk_copy)
    wait_all(m, wv_copy)
    start_all(m, x_copy)
    for copy in own:
        copy.wait()
    both = dot_nn(x_ref[...], w_out[...]).astype(BF16)
    pieces = []
    for group in range(kv_heads):
        pieces.append(both[:, group * HD : (group + 1) * HD])
        pieces.append(both[:, kv_width + group * HD : kv_width + (group + 1) * HD])
    kv_block[...] = jnp.concatenate(pieces, axis=1)
    start_all(n, kv_copy)
    kv_own = pltpu.make_async_copy(
        column_block(kv_block, (me * kv_heads) // n, 2 * HD),
        row_block(kv_out, me, positions), own_sems.at[5],
    )
    kv_own.start()
    kv_own.wait()
    wait_all(m, x_copy)
    wait_all(n, q_copy)
    wait_all(n, g_copy)
    wait_all(n, kv_copy)


def attend_kernel(
    heads, tile,
    q_ref, g_ref, kv_ref, gate_q, gate_k,
    dq_ref, dkv_ref, gc_ref,
    kx, kt, vs, qx, qd, gh, s_buf, d_buf, dk_acc, dv_acc,
):
    length = kv_ref.shape[0]
    scale = HD ** (-0.5)
    keys = kv_ref[:, :HD]
    kt[...] = keys.astype(F32).T.astype(BF16)
    vs[...] = kv_ref[:, HD:]
    dk_acc[...] = jnp.zeros_like(dk_acc)
    dv_acc[...] = jnp.zeros_like(dv_acc)
    lane = lax.broadcasted_iota(jnp.int32, (length, HD), 1)
    for h in range(heads):
        q_head = q_ref[:, h * HD : (h + 1) * HD]
        kx[h] = jnp.concatenate([keys, gate_k[h]], axis=1)
        qx[h] = jnp.concatenate([q_head * jnp.asarray(scale, BF16), gate_q[h]], axis=1)
        mark = jnp.where(lane == h, 1.0, 0.0).astype(BF16)
        qd[h] = jnp.concatenate([q_head, mark], axis=1)
        gh[h] = g_ref[:, h * HD : (h + 1) * HD]
    later = lax.broadcasted_iota(jnp.int32, (tile, tile), 0) > lax.broadcasted_iota(
        jnp.int32, (tile, tile), 1
    )
    every = range(heads)

    def fold(op, a):
        return op(a.reshape(tile // 8, 8, tile), axis=0)

    @pl.loop(0, length // tile)
    def _(i):
        here = pl.ds(pl.multiple_of(i * tile, tile), tile)

        def score(c, tops, diagonal):
            at = pl.ds(pl.multiple_of(c * tile, tile), tile)
            out = []
            for h in every:
                s = dot_nt(kx[h, at, :], qx[h, here, :])
                if diagonal:
                    s = jnp.where(later, -jnp.inf, s)
                s_buf[h, at, :] = s
                out.append(jnp.maximum(tops[h], fold(jnp.max, s)))
            return tuple(out)

        tops = tuple(jnp.full((8, tile), -jnp.inf, F32) for _ in every)
        tops = lax.fori_loop(0, i, lambda c, v: score(c, v, False), tops)
        tops = score(i, tops, True)
        tops = [jnp.max(top, axis=0, keepdims=True) for top in tops]

        def weigh(c, carry):
            at = pl.ds(pl.multiple_of(c * tile, tile), tile)
            out = []
            for h in every:
                total, dots = carry[h]
                d = dot_nt(vs[at, :], gh[h, here, :])
                e = jnp.exp2((s_buf[h, at, :] - tops[h]) * LOG2E)
                s_buf[h, at, :] = e
                d_buf[h, at, :] = d
                out.append((total + fold(jnp.sum, e), dots + fold(jnp.sum, e * d)))
            return tuple(out)

        zero = jnp.zeros((8, tile), F32)
        sums = lax.fori_loop(0, i + 1, weigh, tuple((zero, zero) for _ in every))
        inverse, row_dot = [], []
        for h in every:
            total = jnp.sum(sums[h][0], axis=0, keepdims=True)
            dots = jnp.sum(sums[h][1], axis=0, keepdims=True)
            inv = 1.0 / total
            inverse.append(inv)
            row_dot.append(dots * inv)
            gc_ref[h : h + 1, here] = dots * inv - row_dot[h] * (total * inv)

        def spread(c, carry):
            at = pl.ds(pl.multiple_of(c * tile, tile), tile)
            out = []
            dk = dk_acc[at, :]
            dv = dv_acc[at, :]
            for h in every:
                p = s_buf[h, at, :] * inverse[h]
                low = (p * (d_buf[h, at, :] - row_dot[h])).astype(BF16)
                dv = dv + dot_nn(p.astype(BF16), gh[h, here, :])
                dk = dk + dot_nn(low, qd[h, here, :])
                out.append(carry[h] + dot_nn(kt[:, at], low))
            dk_acc[at, :] = dk
            dv_acc[at, :] = dv
            return tuple(out)

        start = tuple(jnp.zeros((HD, tile), F32) for _ in every)
        grads = lax.fori_loop(0, i + 1, spread, start)
        dq_ref[here, :] = jnp.concatenate([(gr.T * scale) for gr in grads], axis=1).astype(BF16)

    dk = dk_acc[...]
    dkv_ref[...] = jnp.concatenate([dk[:, :HD] * scale, dv_acc[...]], axis=1).astype(BF16)
    columns = dk.T
    gc_ref[...] = gc_ref[...] - columns[HD : HD + heads, :]


def return_kernel(
    n, m, width, kv_heads, reduce_here,
    dq_ref, dkv_ref, x_ref, w_ref,
    gq_out, gx_out, *rest,
):
    if reduce_here:
        (gwk_out, gwv_out, slots, gkv_all, share, parts, mean_block, whole,
         q_sems, kv_sems, gkv_sems, own_sems, rs_sems, ag_sems) = rest
    else:
        share, slots, gkv_all, q_sems, kv_sems, gkv_sems, own_sems = rest
    me, mine = lax.axis_index("sp"), lax.axis_index("dp")
    positions = slots.shape[1]
    kv_width = kv_heads * HD
    greet(n, m)

    def target(k):
        return lax.rem(me + k, n)

    def peer(k):
        return lax.rem(mine + k, m)

    def q_copy(k):
        return remote(
            row_block(dq_ref, target(k), positions),
            column_block(gq_out, me, width), q_sems, k, {"sp": target(k)},
        )

    def kv_copy(k):
        return remote(
            row_block(dkv_ref, target(k), positions), slots.at[me], kv_sems, k,
            {"sp": target(k)},
        )

    def gkv_copy(k):
        return remote(gkv_all.at[mine], gkv_all.at[mine], gkv_sems, k, {"dp": peer(k)})

    start_all(n, kv_copy)
    start_all(n, q_copy)
    kv_own = pltpu.make_async_copy(
        row_block(dkv_ref, me, positions), slots.at[me], own_sems.at[0]
    )
    q_own = pltpu.make_async_copy(
        row_block(dq_ref, me, positions), column_block(gq_out, me, width), own_sems.at[1]
    )
    kv_own.start()
    q_own.start()
    kv_own.wait()
    q_own.wait()
    wait_all(n, kv_copy)
    per = n // kv_heads
    groups = []
    for group in range(kv_heads):
        total = slots[group * per].astype(F32)
        for j in range(1, per):
            total = total + slots[group * per + j].astype(F32)
        groups.append(total)
    gkv = jnp.concatenate(
        [total[:, :HD] for total in groups] + [total[:, HD:] for total in groups], axis=1
    ).astype(BF16)
    gkv_all[mine] = gkv
    start_all(m, gkv_copy)
    gx_out[...] = dot_nt(gkv, w_ref[...]).astype(BF16)
    wait_all(m, gkv_copy)
    total = dot_tn(x_ref[0], gkv_all[0])
    for j in range(1, m):
        total = total + dot_tn(x_ref[j], gkv_all[j])
    share[...] = total.astype(BF16)
    if reduce_here:
        piece = share.shape[0] // n

        def rs_copy(k):
            return remote(
                row_block(share, target(k), piece), parts.at[me], rs_sems, k,
                {"sp": target(k)},
            )

        def ag_copy(k):
            return remote(
                mean_block, row_block(whole, me, piece), ag_sems, k, {"sp": target(k)}
            )

        start_all(n, rs_copy)
        rs_own = pltpu.make_async_copy(row_block(share, me, piece), parts.at[me], own_sems.at[2])
        rs_own.start()
        rs_own.wait()
        wait_all(n, rs_copy)
        total = parts[0].astype(F32)
        for j in range(1, n):
            total = total + parts[j].astype(F32)
        mean_block[...] = total.astype(BF16)
        start_all(n, ag_copy)
        ag_own = pltpu.make_async_copy(mean_block, row_block(whole, me, piece), own_sems.at[3])
        ag_own.start()
        ag_own.wait()
        wait_all(n, ag_copy)
        gwk_out[...] = whole[:, :kv_width].astype(F32)
        gwv_out[...] = whole[:, kv_width:].astype(F32)
    wait_all(n, q_copy)


def split_bits(gate):
    first = lax.reduce_precision(gate, 8, 7)
    second = lax.reduce_precision(gate - first, 8, 7)
    third = lax.reduce_precision(gate - first - second, 8, 7)
    return first, second, third


def per_device(n, m, inputs, w_key, w_value, queries, cotangent, cum_gate):
    seq_count, positions, feature_count = inputs.shape
    rows, kv_width = w_key.shape
    kv_heads = kv_width // HD
    query_width = queries.shape[2]
    width = query_width // n
    heads = width // HD
    length = positions * n
    dma = pltpu.SemaphoreType.DMA

    def params(cid):
        return pltpu.CompilerParams(
            collective_id=cid, has_side_effects=True, vmem_limit_bytes=60 * 1024 * 1024
        )

    def shape(dims, dtype=BF16):
        return jax.ShapeDtypeStruct(dims, dtype)

    def blocks(x):
        if width % LANES == 0:
            return x.reshape(positions, query_width)
        return x.reshape(positions, n, width).transpose(1, 0, 2)

    first, second, third = split_bits(cum_gate[0])
    one = jnp.ones_like(first)
    zero = jnp.zeros_like(first)
    pad = [zero] * (HD - 6)
    gate_q = jnp.stack([one, one, one, first, second, third] + pad, axis=2).astype(BF16)
    gate_k = jnp.stack([-first, -second, -third, one, one, one] + pad, axis=2).astype(BF16)

    q_all, g_all, kv_all, w_all, x_all = pl.pallas_call(
        functools.partial(gather_kernel, n, m, width, kv_heads),
        out_shape=(
            shape((length, width)),
            shape((length, width)),
            shape((length, 2 * HD)),
            shape((rows * m, 2 * kv_width)),
            shape((m, positions, rows)),
        ),
        in_specs=[VMEM] * 5,
        out_specs=(VMEM,) * 5,
        scratch_shapes=[
            pltpu.VMEM((positions, 2 * kv_width), BF16),
            dma((2, n)), dma((2, n)), dma((2, n)),
            dma((2, m)), dma((2, m)), dma((2, m)), dma((6,)),
        ],
        compiler_params=params(0),
        name="gather_heads",
    )(blocks(queries), blocks(cotangent), inputs[0], w_key, w_value)

    tile = 256
    dq, dkv, grad_cum = pl.pallas_call(
        functools.partial(attend_kernel, heads, tile),
        out_shape=(
            shape((length, width)),
            shape((length, 2 * HD)),
            shape((heads, length), F32),
        ),
        in_specs=[VMEM] * 5,
        out_specs=(VMEM,) * 3,
        scratch_shapes=[
            pltpu.VMEM((heads, length, LANES), BF16),
            pltpu.VMEM((HD, length), BF16),
            pltpu.VMEM((length, HD), BF16),
            pltpu.VMEM((heads, length, LANES), BF16),
            pltpu.VMEM((heads, length, LANES), BF16),
            pltpu.VMEM((heads, length, HD), BF16),
            pltpu.VMEM((heads, length, tile), F32),
            pltpu.VMEM((heads, length, tile), F32),
            pltpu.VMEM((length, LANES), F32),
            pltpu.VMEM((length, HD), F32),
        ],
        compiler_params=pltpu.CompilerParams(vmem_limit_bytes=60 * 1024 * 1024),
        name="attend",
    )(q_all, g_all, kv_all, gate_q, gate_k)

    piece = rows // n
    reduce_here = rows % (16 * n) == 0
    gq_shape = (positions, query_width) if width % LANES == 0 else (n, positions, width)
    share_shape = (rows, 2 * kv_width)
    out_shape = [shape(gq_shape), shape((positions, feature_count))]
    scratch = [
        pltpu.VMEM((n, positions, 2 * HD), BF16),
        pltpu.VMEM((m, positions, 2 * kv_width), BF16),
    ]
    sems = [dma((2, n)), dma((2, n)), dma((2, m)), dma((4,))]
    if reduce_here:
        out_shape += [shape((rows, kv_width), F32)] * 2
        scratch += [
            pltpu.VMEM(share_shape, BF16),
            pltpu.VMEM((n, piece, 2 * kv_width), BF16),
            pltpu.VMEM((piece, 2 * kv_width), BF16),
            pltpu.VMEM(share_shape, BF16),
        ]
        sems += [dma((2, n)), dma((2, n))]
    else:
        out_shape += [shape(share_shape)]
    results = pl.pallas_call(
        functools.partial(return_kernel, n, m, width, kv_heads, reduce_here),
        out_shape=tuple(out_shape),
        in_specs=[VMEM] * 4,
        out_specs=(VMEM,) * len(out_shape),
        scratch_shapes=scratch + sems,
        compiler_params=params(1),
        name="return_tokens",
    )(dq, dkv, x_all, w_all)
    grad_queries, grad_input = results[:2]
    if width % LANES:
        grad_queries = grad_queries.transpose(1, 0, 2)
    if reduce_here:
        grad_wk, grad_wv = results[2:]
    else:
        summed = lax.psum(results[2], "sp").astype(F32)
        grad_wk, grad_wv = summed[:, :kv_width], summed[:, kv_width:]
    return (
        grad_input.reshape(inputs.shape),
        grad_queries.reshape(queries.shape),
        grad_cum.reshape(cum_gate.shape),
        grad_wk,
        grad_wv,
    )


def solution(mesh):
    in_specs = (
        P("dp", "sp", None),
        P("dp", None),
        P("dp", None),
        P("dp", "sp", None),
        P("dp", "sp", None),
        P("dp", "sp", None),
    )
    out_specs = (
        P("dp", "sp", None),
        P("dp", "sp", None),
        P("dp", "sp", None),
        P("dp", None),
        P("dp", None),
    )
    body = functools.partial(per_device, mesh.shape["sp"], mesh.shape["dp"])
    return jax.shard_map(
        body, mesh=mesh, in_specs=in_specs, out_specs=out_specs, check_vma=False
    )
```

```python
import functools

import jax
import jax.numpy as jnp
from jax import lax
from jax.experimental import pallas as pl
from jax.experimental.pallas import tpu as pltpu
from jax.sharding import PartitionSpec as P

HD = 64
LANES = 128
LOG2E = 1.4426950408889634
MESH = pl.DeviceIdType.MESH
VMEM = pl.BlockSpec(memory_space=pltpu.VMEM)
BF16 = jnp.bfloat16
F32 = jnp.float32


def dot_nn(a, b):
    return jnp.dot(a, b, preferred_element_type=F32)


def dot_nt(a, b):
    return lax.dot_general(a, b, (((1,), (1,)), ((), ())), preferred_element_type=F32)


def dot_tn(a, b):
    return lax.dot_general(a, b, (((0,), (0,)), ((), ())), preferred_element_type=F32)


def greet(n, m):
    me, mine = lax.axis_index("sp"), lax.axis_index("dp")
    barrier = pltpu.get_barrier_semaphore()

    @pl.loop(1, n)
    def _(k):
        pl.semaphore_signal(
            barrier, inc=1, device_id={"sp": lax.rem(me + k, n)}, device_id_type=MESH
        )

    @pl.loop(1, m)
    def _(k):
        pl.semaphore_signal(
            barrier, inc=1, device_id={"dp": lax.rem(mine + k, m)}, device_id_type=MESH
        )

    pl.semaphore_wait(barrier, n + m - 2)


def start_all(n, make):
    @pl.loop(1, n)
    def _(k):
        make(k).start()


def wait_all(n, make):
    @pl.loop(1, n)
    def _(k):
        make(k).wait()


def remote(src, dst, sems, k, device):
    return pltpu.make_async_remote_copy(
        src_ref=src,
        dst_ref=dst,
        send_sem=sems.at[0, k],
        recv_sem=sems.at[1, k],
        device_id=device,
        device_id_type=MESH,
    )


def column_block(ref, j, width):
    if len(ref.shape) == 3:
        return ref.at[j]
    return ref.at[:, pl.ds(pl.multiple_of(j * width, LANES), width)]


def row_block(ref, j, rows):
    return ref.at[pl.ds(pl.multiple_of(j * rows, 16), rows)]


def gather_kernel(
    n, m, width, kv_heads,
    q_ref, g_ref, x_ref, wk_ref, wv_ref,
    q_out, g_out, kv_out, w_out, x_out,
    kv_block, q_sems, g_sems, kv_sems, mate_sems, wk_sems, wv_sems, x_sems, own_sems,
):
    me, mine = lax.axis_index("sp"), lax.axis_index("dp")
    per = n // kv_heads
    plane, member = me // per, lax.rem(me, per)
    positions = x_ref.shape[0]
    rows, kv_width = wk_ref.shape
    greet(n, m)

    def target(k):
        return lax.rem(me + k, n)

    def peer(k):
        return lax.rem(mine + k, m)

    def wk_copy(k):
        dst = row_block(w_out, mine, rows).at[:, pl.ds(0, kv_width)]
        return remote(wk_ref, dst, wk_sems, k, {"dp": peer(k)})

    def wv_copy(k):
        dst = row_block(w_out, mine, rows).at[:, pl.ds(kv_width, kv_width)]
        return remote(wv_ref, dst, wv_sems, k, {"dp": peer(k)})

    def x_copy(k):
        return remote(
            column_block(x_ref, peer(k), rows), x_out.at[mine], x_sems, k, {"dp": peer(k)}
        )

    def q_copy(k):
        return remote(
            column_block(q_ref, target(k), width),
            row_block(q_out, me, positions), q_sems, k, {"sp": target(k)},
        )

    def g_copy(k):
        return remote(
            column_block(g_ref, target(k), width),
            row_block(g_out, me, positions), g_sems, k, {"sp": target(k)},
        )

    def kv_copy(k):
        group = lax.rem(plane + k, kv_heads)
        return remote(
            column_block(kv_block, group, 2 * HD),
            row_block(kv_out, me, positions), kv_sems, k, {"sp": group * per + member},
        )

    def mate_copy(k, step):
        source = lax.rem(plane - step + kv_heads, kv_heads) * per + member
        rows_of = row_block(kv_out, source, positions)
        return remote(
            rows_of, rows_of, mate_sems.at[step], k,
            {"sp": plane * per + lax.rem(member + k, per)},
        )

    own = [
        pltpu.make_async_copy(
            wk_ref, row_block(w_out, mine, rows).at[:, pl.ds(0, kv_width)], own_sems.at[0]
        ),
        pltpu.make_async_copy(
            wv_ref, row_block(w_out, mine, rows).at[:, pl.ds(kv_width, kv_width)], own_sems.at[1]
        ),
        pltpu.make_async_copy(column_block(x_ref, mine, rows), x_out.at[mine], own_sems.at[2]),
        pltpu.make_async_copy(
            column_block(q_ref, me, width), row_block(q_out, me, positions), own_sems.at[3]
        ),
        pltpu.make_async_copy(
            column_block(g_ref, me, width), row_block(g_out, me, positions), own_sems.at[4]
        ),
    ]
    start_all(m, wk_copy)
    start_all(m, wv_copy)
    start_all(n, q_copy)
    for copy in own:
        copy.start()
    wait_all(m, wk_copy)
    wait_all(m, wv_copy)
    for copy in own:
        copy.wait()
    both = dot_nn(x_ref[...], w_out[...]).astype(BF16)
    pieces = []
    for group in range(kv_heads):
        pieces.append(both[:, group * HD : (group + 1) * HD])
        pieces.append(both[:, kv_width + group * HD : kv_width + (group + 1) * HD])
    kv_block[...] = jnp.concatenate(pieces, axis=1)
    start_all(kv_heads, kv_copy)
    kv_own = pltpu.make_async_copy(
        column_block(kv_block, plane, 2 * HD),
        row_block(kv_out, me, positions), own_sems.at[5],
    )
    kv_own.start()
    start_all(n, g_copy)
    start_all(m, x_copy)
    kv_own.wait()
    start_all(per, lambda k: mate_copy(k, 0))

    @pl.loop(1, kv_heads)
    def _(step):
        kv_copy(step).wait()
        start_all(per, lambda k: mate_copy(k, step))

    wait_all(m, x_copy)
    wait_all(n, q_copy)
    wait_all(n, g_copy)

    @pl.loop(0, kv_heads)
    def _(step):
        wait_all(per, lambda k: mate_copy(k, step))


def split_bits(gate):
    first = gate.astype(BF16).astype(F32)
    second = (gate - first).astype(BF16).astype(F32)
    third = (gate - first - second).astype(BF16).astype(F32)
    return first, second, third


def attend_kernel(
    n, m, width, kv_heads, tile, reduce_here,
    q_ref, g_ref, kv_ref, gate_ref, x_ref, w_ref,
    gq_out, gx_out, gc_ref, *rest,
):
    if reduce_here:
        (gwk_out, gwv_out, *rest, share, parts, mean_block, whole, rs_sems, ag_sems) = rest
    else:
        share, *rest = rest
    (kx, kt, vs, qx, qd, gh, s_buf, d_buf, dk_acc, dv_acc, dq_buf, dkv_buf,
     slots, sums_buf, groups_buf, gkv_all,
     q_sems, mate_sems, group_sems, gkv_sems, own_sems) = rest
    me, mine = lax.axis_index("sp"), lax.axis_index("dp")
    heads = width // HD
    length = kv_ref.shape[0]
    positions = gx_out.shape[0]
    kv_width = kv_heads * HD
    per = n // kv_heads
    plane, member = me // per, lax.rem(me, per)
    scale = HD ** (-0.5)
    greet(n, m)

    def target(k):
        return lax.rem(me + k, n)

    def peer(k):
        return lax.rem(mine + k, m)

    def q_copy(k):
        return remote(
            row_block(dq_buf, target(k), positions),
            column_block(gq_out, me, width), q_sems, k, {"sp": target(k)},
        )

    def mate_copy(k, a):
        to = lax.rem(member + k, per)
        return remote(
            row_block(dkv_buf, a * per + to, positions), slots.at[member, a],
            mate_sems.at[a], k, {"sp": plane * per + to},
        )

    def group_copy(k):
        a = lax.rem(plane + k, kv_heads)
        return remote(
            sums_buf.at[a], groups_buf.at[plane], group_sems, k, {"sp": a * per + member}
        )

    def gkv_copy(k):
        return remote(gkv_all.at[mine], gkv_all.at[mine], gkv_sems, k, {"dp": peer(k)})

    q_own = pltpu.make_async_copy(
        row_block(dq_buf, me, positions), column_block(gq_out, me, width), own_sems.at[0]
    )

    def send_tile(i):
        for part in range(tile // positions):
            j = i * (tile // positions) + part
            k = lax.rem(j - me + n, n)
            a, b = j // per, lax.rem(j, per)
            km = lax.rem(b - member + per, per)

            @pl.when(km != 0)
            def _():
                mate_copy(km, a).start()

            @pl.when(k != 0)
            def _():
                q_copy(k).start()

    keys = kv_ref[:, :HD]
    kt[...] = keys.astype(F32).T.astype(BF16)
    vs[...] = kv_ref[:, HD:]
    dk_acc[...] = jnp.zeros_like(dk_acc)
    dv_acc[...] = jnp.zeros_like(dv_acc)
    lane = lax.broadcasted_iota(jnp.int32, (length, HD), 1)
    ones = jnp.ones((3, length), F32)
    blank = jnp.zeros((HD - 6, length), F32)
    for h in range(heads):
        three = jnp.concatenate(split_bits(gate_ref[h : h + 1, :]), axis=0)
        gates = jnp.concatenate([ones, three, blank, -three, ones, blank], axis=0).T.astype(BF16)
        q_head = q_ref[:, h * HD : (h + 1) * HD]
        kx[h] = jnp.concatenate([keys, gates[:, HD:]], axis=1)
        qx[h] = jnp.concatenate([q_head * jnp.asarray(scale, BF16), gates[:, :HD]], axis=1)
        mark = jnp.where(lane == h, 1.0, 0.0).astype(BF16)
        qd[h] = jnp.concatenate([q_head, mark], axis=1)
        gh[h] = g_ref[:, h * HD : (h + 1) * HD]
    later = lax.broadcasted_iota(jnp.int32, (tile, tile), 0) > lax.broadcasted_iota(
        jnp.int32, (tile, tile), 1
    )
    every = range(heads)

    def fold(op, a):
        return op(a.reshape(tile // 8, 8, tile), axis=0)

    tiles = length // tile

    @pl.loop(0, tiles)
    def _(turn):
        i = tiles - 1 - turn
        here = pl.ds(pl.multiple_of(i * tile, tile), tile)

        def score(c, tops, diagonal):
            at = pl.ds(pl.multiple_of(c * tile, tile), tile)
            out = []
            for h in every:
                s = dot_nt(kx[h, at, :], qx[h, here, :])
                if diagonal:
                    s = jnp.where(later, -jnp.inf, s)
                s_buf[h, at, :] = s
                out.append(jnp.maximum(tops[h], fold(jnp.max, s)))
            return tuple(out)

        tops = tuple(jnp.full((8, tile), -jnp.inf, F32) for _ in every)
        tops = lax.fori_loop(0, i, lambda c, v: score(c, v, False), tops)
        tops = score(i, tops, True)
        tops = [jnp.max(top, axis=0, keepdims=True) for top in tops]

        def weigh(c, carry):
            at = pl.ds(pl.multiple_of(c * tile, tile), tile)
            out = []
            for h in every:
                total, dots = carry[h]
                d = dot_nt(vs[at, :], gh[h, here, :])
                e = jnp.exp2((s_buf[h, at, :] - tops[h]) * LOG2E)
                s_buf[h, at, :] = e
                d_buf[h, at, :] = d
                out.append((total + fold(jnp.sum, e), dots + fold(jnp.sum, e * d)))
            return tuple(out)

        zero = jnp.zeros((8, tile), F32)
        sums = lax.fori_loop(0, i + 1, weigh, tuple((zero, zero) for _ in every))
        inverse, row_dot = [], []
        for h in every:
            total = jnp.sum(sums[h][0], axis=0, keepdims=True)
            dots = jnp.sum(sums[h][1], axis=0, keepdims=True)
            inv = 1.0 / total
            inverse.append(inv)
            row_dot.append(dots * inv)
            gc_ref[h : h + 1, here] = dots * inv - row_dot[h] * (total * inv)

        def spread(c, carry):
            at = pl.ds(pl.multiple_of(c * tile, tile), tile)
            out = []
            dk = dk_acc[at, :]
            dv = dv_acc[at, :]
            for h in every:
                p = s_buf[h, at, :] * inverse[h]
                low = (p * (d_buf[h, at, :] - row_dot[h])).astype(BF16)
                dv = dv + dot_nn(p.astype(BF16), gh[h, here, :])
                dk = dk + dot_nn(low, qd[h, here, :])
                out.append(carry[h] + dot_nn(kt[:, at], low))
            dk_acc[at, :] = dk
            dv_acc[at, :] = dv
            return tuple(out)

        start = tuple(jnp.zeros((HD, tile), F32) for _ in every)
        grads = lax.fori_loop(0, i + 1, spread, start)
        dq_buf[here, :] = jnp.concatenate([gr.T * scale for gr in grads], axis=1).astype(BF16)
        dkv_buf[here, :] = jnp.concatenate(
            [dk_acc[here, :][:, :HD] * scale, dv_acc[here, :]], axis=1
        ).astype(BF16)

        @pl.when(turn > 0)
        def _():
            send_tile(i + 1)

    send_tile(0)
    q_own.start()
    columns = dk_acc[...].T
    gc_ref[...] = gc_ref[...] - columns[HD : HD + heads, :]

    @pl.loop(0, kv_heads)
    def _(step):
        a = lax.rem(plane + 1 + step, kv_heads)
        wait_all(per, lambda k: mate_copy(k, a))
        rows_of = row_block(dkv_buf, a * per + member, positions)
        total = rows_of[...].astype(F32)
        for k in range(1, per):
            total = total + slots[lax.rem(member + k, per), a].astype(F32)
        sums_buf[a] = total.astype(BF16)

        @pl.when(step < kv_heads - 1)
        def _():
            group_copy(step + 1).start()

    groups_buf[plane] = sums_buf[plane]
    wait_all(kv_heads, group_copy)
    groups = [groups_buf[group] for group in range(kv_heads)]
    gkv = jnp.concatenate(
        [total[:, :HD] for total in groups] + [total[:, HD:] for total in groups], axis=1
    )
    gkv_all[mine] = gkv
    start_all(m, gkv_copy)
    gx_out[...] = dot_nt(gkv, w_ref[...]).astype(BF16)
    wait_all(m, gkv_copy)
    total = dot_tn(x_ref[0], gkv_all[0])
    for j in range(1, m):
        total = total + dot_tn(x_ref[j], gkv_all[j])
    share[...] = total.astype(BF16)
    if reduce_here:
        piece = share.shape[0] // n

        def rs_copy(k):
            return remote(
                row_block(share, target(k), piece), parts.at[me], rs_sems, k,
                {"sp": target(k)},
            )

        def ag_copy(k):
            return remote(
                mean_block, row_block(whole, me, piece), ag_sems, k, {"sp": target(k)}
            )

        start_all(n, rs_copy)
        rs_own = pltpu.make_async_copy(row_block(share, me, piece), parts.at[me], own_sems.at[1])
        rs_own.start()
        rs_own.wait()
        wait_all(n, rs_copy)
        total = parts[0].astype(F32)
        for j in range(1, n):
            total = total + parts[j].astype(F32)
        mean_block[...] = total.astype(BF16)
        start_all(n, ag_copy)
        ag_own = pltpu.make_async_copy(mean_block, row_block(whole, me, piece), own_sems.at[2])
        ag_own.start()
        ag_own.wait()
        wait_all(n, ag_copy)
        gwk_out[...] = whole[:, :kv_width].astype(F32)
        gwv_out[...] = whole[:, kv_width:].astype(F32)
    q_own.wait()
    wait_all(n, q_copy)


def per_device(n, m, inputs, w_key, w_value, queries, cotangent, cum_gate):
    seq_count, positions, feature_count = inputs.shape
    rows, kv_width = w_key.shape
    kv_heads = kv_width // HD
    query_width = queries.shape[2]
    width = query_width // n
    heads = width // HD
    length = positions * n
    dma = pltpu.SemaphoreType.DMA

    def params(cid):
        return pltpu.CompilerParams(
            collective_id=cid, has_side_effects=True, vmem_limit_bytes=60 * 1024 * 1024
        )

    def shape(dims, dtype=BF16):
        return jax.ShapeDtypeStruct(dims, dtype)

    def blocks(x):
        if width % LANES == 0:
            return x.reshape(positions, query_width)
        return x.reshape(positions, n, width).transpose(1, 0, 2)

    q_all, g_all, kv_all, w_all, x_all = pl.pallas_call(
        functools.partial(gather_kernel, n, m, width, kv_heads),
        out_shape=(
            shape((length, width)),
            shape((length, width)),
            shape((length, 2 * HD)),
            shape((rows * m, 2 * kv_width)),
            shape((m, positions, rows)),
        ),
        in_specs=[VMEM] * 5,
        out_specs=(VMEM,) * 5,
        scratch_shapes=[
            pltpu.VMEM((positions, 2 * kv_width), BF16),
            dma((2, n)), dma((2, n)), dma((2, kv_heads)), dma((kv_heads, 2, n // kv_heads)),
            dma((2, m)), dma((2, m)), dma((2, m)), dma((6,)),
        ],
        compiler_params=params(0),
        name="gather_heads",
    )(blocks(queries), blocks(cotangent), inputs[0], w_key, w_value)

    tile = max(256, positions)
    piece = rows // n
    reduce_here = rows % (16 * n) == 0
    gq_shape = (positions, query_width) if width % LANES == 0 else (n, positions, width)
    share_shape = (rows, 2 * kv_width)
    per = n // kv_heads
    out_shape = [
        shape(gq_shape), shape((positions, feature_count)), shape((heads, length), F32)
    ]
    scratch = [
        pltpu.VMEM((heads, length, LANES), BF16),
        pltpu.VMEM((HD, length), BF16),
        pltpu.VMEM((length, HD), BF16),
        pltpu.VMEM((heads, length, LANES), BF16),
        pltpu.VMEM((heads, length, LANES), BF16),
        pltpu.VMEM((heads, length, HD), BF16),
        pltpu.VMEM((heads, length, tile), F32),
        pltpu.VMEM((heads, length, tile), F32),
        pltpu.VMEM((length, LANES), F32),
        pltpu.VMEM((length, HD), F32),
        pltpu.VMEM((length, width), BF16),
        pltpu.VMEM((length, 2 * HD), BF16),
        pltpu.VMEM((per, kv_heads, positions, 2 * HD), BF16),
        pltpu.VMEM((kv_heads, positions, 2 * HD), BF16),
        pltpu.VMEM((kv_heads, positions, 2 * HD), BF16),
        pltpu.VMEM((m, positions, 2 * kv_width), BF16),
        dma((2, n)), dma((kv_heads, 2, per)), dma((2, kv_heads)), dma((2, m)), dma((3,)),
    ]
    if reduce_here:
        out_shape += [shape((rows, kv_width), F32)] * 2
        scratch += [
            pltpu.VMEM(share_shape, BF16),
            pltpu.VMEM((n, piece, 2 * kv_width), BF16),
            pltpu.VMEM((piece, 2 * kv_width), BF16),
            pltpu.VMEM(share_shape, BF16),
            dma((2, n)), dma((2, n)),
        ]
    else:
        out_shape += [shape(share_shape)]
    results = pl.pallas_call(
        functools.partial(attend_kernel, n, m, width, kv_heads, tile, reduce_here),
        out_shape=tuple(out_shape),
        in_specs=[VMEM] * 6,
        out_specs=(VMEM,) * len(out_shape),
        scratch_shapes=scratch,
        compiler_params=params(1),
        name="attend_return",
    )(q_all, g_all, kv_all, cum_gate[0], x_all, w_all)
    grad_queries, grad_input, grad_cum = results[:3]
    if width % LANES:
        grad_queries = grad_queries.transpose(1, 0, 2)
    if reduce_here:
        grad_wk, grad_wv = results[3:]
    else:
        summed = lax.psum(results[3], "sp").astype(F32)
        grad_wk, grad_wv = summed[:, :kv_width], summed[:, kv_width:]
    return (
        grad_input.reshape(inputs.shape),
        grad_queries.reshape(queries.shape),
        grad_cum.reshape(cum_gate.shape),
        grad_wk,
        grad_wv,
    )


def solution(mesh):
    in_specs = (
        P("dp", "sp", None),
        P("dp", None),
        P("dp", None),
        P("dp", "sp", None),
        P("dp", "sp", None),
        P("dp", "sp", None),
    )
    out_specs = (
        P("dp", "sp", None),
        P("dp", "sp", None),
        P("dp", "sp", None),
        P("dp", None),
        P("dp", None),
    )
    body = functools.partial(per_device, mesh.shape["sp"], mesh.shape["dp"])
    return jax.shard_map(
        body, mesh=mesh, in_specs=in_specs, out_specs=out_specs, check_vma=False
    )
```

```python
import functools

import jax
import jax.numpy as jnp
from jax import lax
from jax.experimental import pallas as pl
from jax.experimental.pallas import tpu as pltpu
from jax.sharding import PartitionSpec as P

HD = 64
LANES = 128
LOG2E = 1.4426950408889634
MESH = pl.DeviceIdType.MESH
VMEM = pl.BlockSpec(memory_space=pltpu.VMEM)
BF16 = jnp.bfloat16
F32 = jnp.float32


def dot_nn(a, b):
    return jnp.dot(a, b, preferred_element_type=F32)


def dot_nt(a, b):
    return lax.dot_general(a, b, (((1,), (1,)), ((), ())), preferred_element_type=F32)


def dot_tn(a, b):
    return lax.dot_general(a, b, (((0,), (0,)), ((), ())), preferred_element_type=F32)


def greet(n, m):
    me, mine = lax.axis_index("sp"), lax.axis_index("dp")
    barrier = pltpu.get_barrier_semaphore()

    @pl.loop(1, n)
    def _(k):
        pl.semaphore_signal(
            barrier, inc=1, device_id={"sp": lax.rem(me + k, n)}, device_id_type=MESH
        )

    @pl.loop(1, m)
    def _(k):
        pl.semaphore_signal(
            barrier, inc=1, device_id={"dp": lax.rem(mine + k, m)}, device_id_type=MESH
        )

    pl.semaphore_wait(barrier, n + m - 2)


def start_all(n, make):
    @pl.loop(1, n)
    def _(k):
        make(k).start()


def wait_all(n, make):
    @pl.loop(1, n)
    def _(k):
        make(k).wait()


def remote(src, dst, sems, k, device):
    return pltpu.make_async_remote_copy(
        src_ref=src,
        dst_ref=dst,
        send_sem=sems.at[0, k],
        recv_sem=sems.at[1, k],
        device_id=device,
        device_id_type=MESH,
    )


def column_block(ref, j, width):
    if len(ref.shape) == 3:
        return ref.at[j]
    return ref.at[:, pl.ds(pl.multiple_of(j * width, LANES), width)]


def row_block(ref, j, rows):
    return ref.at[pl.ds(pl.multiple_of(j * rows, 16), rows)]


def split_bits(gate):
    first = gate.astype(BF16).astype(F32)
    second = (gate - first).astype(BF16).astype(F32)
    third = (gate - first - second).astype(BF16).astype(F32)
    return first, second, third


def attend_kernel(
    n, m, width, kv_heads, tile, reduce_here,
    q_ref, g_ref, gate_ref, x_ref, wk_ref, wv_ref,
    gq_out, gx_out, gc_ref, *rest,
):
    if reduce_here:
        (gw_out, *rest, share, parts, rs_sum, rs_groups, whole,
         rs_mate_sems, rs_sems, ag_sems, ag_mate_sems) = rest
    else:
        share, *rest = rest
    (q_all, g_all, kv_all, w_all, x_all, kv_block,
     qi_sems, g_sems, kvi_sems, matei_sems, wk_sems, wv_sems, x_sems, owni_sems,
     kx, kt, vs, qx, qd, gh, s_buf, d_buf, dk_acc, dv_acc, dq_buf, dkv_buf,
     slots, sums_buf, groups_buf, gkv_all,
     q_sems, mate_sems, group_sems, gkv_sems, own_sems) = rest
    me, mine = lax.axis_index("sp"), lax.axis_index("dp")
    heads = width // HD
    length = kv_all.shape[0]
    positions = x_ref.shape[0]
    rows, kv_width = wk_ref.shape
    per = n // kv_heads
    plane, member = me // per, lax.rem(me, per)
    scale = HD ** (-0.5)
    greet(n, m)

    def target(k):
        return lax.rem(me + k, n)

    def peer(k):
        return lax.rem(mine + k, m)

    def wk_copy(k):
        dst = row_block(w_all, mine, rows).at[:, pl.ds(0, kv_width)]
        return remote(wk_ref, dst, wk_sems, k, {"dp": peer(k)})

    def wv_copy(k):
        dst = row_block(w_all, mine, rows).at[:, pl.ds(kv_width, kv_width)]
        return remote(wv_ref, dst, wv_sems, k, {"dp": peer(k)})

    def x_copy(k):
        return remote(
            column_block(x_ref, peer(k), rows), x_all.at[mine], x_sems, k, {"dp": peer(k)}
        )

    def qi_copy(k):
        return remote(
            column_block(q_ref, target(k), width),
            row_block(q_all, me, positions), qi_sems, k, {"sp": target(k)},
        )

    def g_copy(k):
        return remote(
            column_block(g_ref, target(k), width),
            row_block(g_all, me, positions), g_sems, k, {"sp": target(k)},
        )

    def kvi_copy(k):
        group = lax.rem(plane + k, kv_heads)
        return remote(
            column_block(kv_block, group, 2 * HD),
            row_block(kv_all, me, positions), kvi_sems, k, {"sp": group * per + member},
        )

    def matei_copy(k, step):
        source = lax.rem(plane - step + kv_heads, kv_heads) * per + member
        rows_of = row_block(kv_all, source, positions)
        return remote(
            rows_of, rows_of, matei_sems.at[step], k,
            {"sp": plane * per + lax.rem(member + k, per)},
        )

    own = [
        pltpu.make_async_copy(
            wk_ref, row_block(w_all, mine, rows).at[:, pl.ds(0, kv_width)], owni_sems.at[0]
        ),
        pltpu.make_async_copy(
            wv_ref, row_block(w_all, mine, rows).at[:, pl.ds(kv_width, kv_width)], owni_sems.at[1]
        ),
        pltpu.make_async_copy(column_block(x_ref, mine, rows), x_all.at[mine], owni_sems.at[2]),
        pltpu.make_async_copy(
            column_block(q_ref, me, width), row_block(q_all, me, positions), owni_sems.at[3]
        ),
        pltpu.make_async_copy(
            column_block(g_ref, me, width), row_block(g_all, me, positions), owni_sems.at[4]
        ),
    ]
    start_all(m, wk_copy)
    start_all(m, wv_copy)
    start_all(n, qi_copy)
    for copy in own:
        copy.start()
    wait_all(m, wk_copy)
    wait_all(m, wv_copy)
    for copy in own:
        copy.wait()
    both = dot_nn(x_ref[...], w_all[...]).astype(BF16)
    pieces = []
    for group in range(kv_heads):
        pieces.append(both[:, group * HD : (group + 1) * HD])
        pieces.append(both[:, kv_width + group * HD : kv_width + (group + 1) * HD])
    kv_block[...] = jnp.concatenate(pieces, axis=1)
    start_all(kv_heads, kvi_copy)
    kv_own = pltpu.make_async_copy(
        column_block(kv_block, plane, 2 * HD),
        row_block(kv_all, me, positions), owni_sems.at[5],
    )
    kv_own.start()
    start_all(n, g_copy)
    start_all(m, x_copy)
    kv_own.wait()
    start_all(per, lambda k: matei_copy(k, 0))

    @pl.loop(1, kv_heads)
    def _(step):
        kvi_copy(step).wait()
        start_all(per, lambda k: matei_copy(k, step))

    def q_copy(k):
        return remote(
            row_block(dq_buf, target(k), positions),
            column_block(gq_out, me, width), q_sems, k, {"sp": target(k)},
        )

    def mate_copy(k, a):
        to = lax.rem(member + k, per)
        return remote(
            row_block(dkv_buf, a * per + to, positions), slots.at[member, a],
            mate_sems.at[a], k, {"sp": plane * per + to},
        )

    def group_copy(k):
        a = lax.rem(plane + k, kv_heads)
        return remote(
            sums_buf.at[a], groups_buf.at[plane], group_sems, k, {"sp": a * per + member}
        )

    def gkv_copy(k):
        return remote(gkv_all.at[mine], gkv_all.at[mine], gkv_sems, k, {"dp": peer(k)})

    q_own = pltpu.make_async_copy(
        row_block(dq_buf, me, positions), column_block(gq_out, me, width), own_sems.at[0]
    )

    def send_tile(i):
        for part in range(tile // positions):
            j = i * (tile // positions) + part
            k = lax.rem(j - me + n, n)
            a, b = j // per, lax.rem(j, per)
            km = lax.rem(b - member + per, per)

            @pl.when(km != 0)
            def _():
                mate_copy(km, a).start()

            @pl.when(k != 0)
            def _():
                q_copy(k).start()

    lane = lax.broadcasted_iota(jnp.int32, (length, HD), 1)
    ones = jnp.ones((3, length), F32)
    blank = jnp.zeros((HD - 6, length), F32)
    dk_acc[...] = jnp.zeros_like(dk_acc)
    dv_acc[...] = jnp.zeros_like(dv_acc)
    wait_all(n, qi_copy)
    for h in range(heads):
        three = jnp.concatenate(split_bits(gate_ref[h : h + 1, :]), axis=0)
        gates = jnp.concatenate([ones, three, blank, -three, ones, blank], axis=0).T.astype(BF16)
        q_head = q_all[:, h * HD : (h + 1) * HD]
        kx[h, :, HD:] = gates[:, HD:]
        qx[h] = jnp.concatenate([q_head * jnp.asarray(scale, BF16), gates[:, :HD]], axis=1)
        mark = jnp.where(lane == h, 1.0, 0.0).astype(BF16)
        qd[h] = jnp.concatenate([q_head, mark], axis=1)
    wait_all(n, g_copy)
    for h in range(heads):
        gh[h] = g_all[:, h * HD : (h + 1) * HD]

    @pl.loop(0, kv_heads)
    def _(step):
        wait_all(per, lambda k: matei_copy(k, step))

    wait_all(m, x_copy)
    keys = kv_all[:, :HD]
    kt[...] = keys.astype(F32).T.astype(BF16)
    vs[...] = kv_all[:, HD:]
    for h in range(heads):
        kx[h, :, :HD] = keys
    later = lax.broadcasted_iota(jnp.int32, (tile, tile), 0) > lax.broadcasted_iota(
        jnp.int32, (tile, tile), 1
    )
    every = range(heads)

    def fold(op, a):
        return op(a.reshape(tile // 8, 8, tile), axis=0)

    tiles = length // tile

    @pl.loop(0, tiles)
    def _(turn):
        i = tiles - 1 - turn
        here = pl.ds(pl.multiple_of(i * tile, tile), tile)

        def score(c, tops, diagonal):
            at = pl.ds(pl.multiple_of(c * tile, tile), tile)
            out = []
            for h in every:
                s = dot_nt(kx[h, at, :], qx[h, here, :])
                if diagonal:
                    s = jnp.where(later, -jnp.inf, s)
                s_buf[h, at, :] = s
                out.append(jnp.maximum(tops[h], fold(jnp.max, s)))
            return tuple(out)

        tops = tuple(jnp.full((8, tile), -jnp.inf, F32) for _ in every)
        tops = lax.fori_loop(0, i, lambda c, v: score(c, v, False), tops)
        tops = score(i, tops, True)
        tops = [jnp.max(top, axis=0, keepdims=True) for top in tops]

        def weigh(c, carry):
            at = pl.ds(pl.multiple_of(c * tile, tile), tile)
            out = []
            for h in every:
                total, dots = carry[h]
                d = dot_nt(vs[at, :], gh[h, here, :])
                e = jnp.exp2((s_buf[h, at, :] - tops[h]) * LOG2E)
                s_buf[h, at, :] = e
                d_buf[h, at, :] = d
                out.append((total + fold(jnp.sum, e), dots + fold(jnp.sum, e * d)))
            return tuple(out)

        zero = jnp.zeros((8, tile), F32)
        sums = lax.fori_loop(0, i + 1, weigh, tuple((zero, zero) for _ in every))
        inverse, row_dot = [], []
        for h in every:
            total = jnp.sum(sums[h][0], axis=0, keepdims=True)
            dots = jnp.sum(sums[h][1], axis=0, keepdims=True)
            inv = 1.0 / total
            inverse.append(inv)
            row_dot.append(dots * inv)
            gc_ref[h : h + 1, here] = dots * inv - row_dot[h] * (total * inv)

        def spread(c, carry):
            at = pl.ds(pl.multiple_of(c * tile, tile), tile)
            out = []
            dk = dk_acc[at, :]
            dv = dv_acc[at, :]
            for h in every:
                p = s_buf[h, at, :] * inverse[h]
                low = (p * (d_buf[h, at, :] - row_dot[h])).astype(BF16)
                dv = dv + dot_nn(p.astype(BF16), gh[h, here, :])
                dk = dk + dot_nn(low, qd[h, here, :])
                out.append(carry[h] + dot_nn(kt[:, at], low))
            dk_acc[at, :] = dk
            dv_acc[at, :] = dv
            return tuple(out)

        start = tuple(jnp.zeros((HD, tile), F32) for _ in every)
        grads = lax.fori_loop(0, i + 1, spread, start)
        dq_buf[here, :] = jnp.concatenate([gr.T * scale for gr in grads], axis=1).astype(BF16)
        dkv_buf[here, :] = jnp.concatenate(
            [dk_acc[here, :][:, :HD] * scale, dv_acc[here, :]], axis=1
        ).astype(BF16)

        @pl.when(turn > 0)
        def _():
            send_tile(i + 1)

    send_tile(0)
    q_own.start()
    columns = dk_acc[...].T
    gc_ref[...] = gc_ref[...] - columns[HD : HD + heads, :]

    @pl.loop(0, kv_heads)
    def _(step):
        a = lax.rem(plane + 1 + step, kv_heads)
        wait_all(per, lambda k: mate_copy(k, a))
        rows_of = row_block(dkv_buf, a * per + member, positions)
        total = rows_of[...].astype(F32)
        for k in range(1, per):
            total = total + slots[lax.rem(member + k, per), a].astype(F32)
        sums_buf[a] = total.astype(BF16)

        @pl.when(step < kv_heads - 1)
        def _():
            group_copy(step + 1).start()

    groups_buf[plane] = sums_buf[plane]
    wait_all(kv_heads, group_copy)
    groups = [groups_buf[group] for group in range(kv_heads)]
    gkv = jnp.concatenate(
        [total[:, :HD] for total in groups] + [total[:, HD:] for total in groups], axis=1
    )
    gkv_all[mine] = gkv
    start_all(m, gkv_copy)
    gx_out[...] = dot_nt(gkv, w_all[...]).astype(BF16)
    wait_all(m, gkv_copy)
    total = dot_tn(x_all[0], gkv_all[0])
    for j in range(1, m):
        total = total + dot_tn(x_all[j], gkv_all[j])
    share[...] = total.astype(BF16)
    if reduce_here:
        piece = rows // n

        def rs_mate_copy(k, a):
            to = lax.rem(member + k, per)
            return remote(
                row_block(share, a * per + to, piece), parts.at[member, a],
                rs_mate_sems.at[a], k, {"sp": plane * per + to},
            )

        def rs_copy(k):
            a = lax.rem(plane + k, kv_heads)
            return remote(
                rs_sum.at[a], rs_groups.at[plane], rs_sems, k, {"sp": a * per + member}
            )

        def ag_copy(k):
            block = row_block(whole, me, piece)
            to = lax.rem(plane + k, kv_heads) * per + member
            return remote(block, block, ag_sems, k, {"sp": to})

        def ag_mate_copy(k, step):
            source = lax.rem(plane - step + kv_heads, kv_heads) * per + member
            block = row_block(whole, source, piece)
            to = plane * per + lax.rem(member + k, per)
            return remote(block, block, ag_mate_sems.at[step], k, {"sp": to})

        @pl.loop(0, kv_heads)
        def _(step):
            start_all(per, lambda k: rs_mate_copy(k, lax.rem(plane + 1 + step, kv_heads)))

        @pl.loop(0, kv_heads)
        def _(step):
            a = lax.rem(plane + 1 + step, kv_heads)
            wait_all(per, lambda k: rs_mate_copy(k, a))
            total = row_block(share, a * per + member, piece)[...].astype(F32)
            for k in range(1, per):
                total = total + parts[lax.rem(member + k, per), a].astype(F32)
            rs_sum[a] = total.astype(BF16)

            @pl.when(step < kv_heads - 1)
            def _():
                rs_copy(step + 1).start()

        total = rs_sum[plane].astype(F32)
        for k in range(1, kv_heads):
            rs_copy(k).wait()
            total = total + rs_groups[lax.rem(plane - k + kv_heads, kv_heads)].astype(F32)
        row_block(whole, me, piece)[...] = total.astype(BF16)
        start_all(kv_heads, ag_copy)
        start_all(per, lambda k: ag_mate_copy(k, 0))

        @pl.loop(1, kv_heads)
        def _(step):
            ag_copy(step).wait()
            start_all(per, lambda k: ag_mate_copy(k, step))

        @pl.loop(0, kv_heads)
        def _(step):
            wait_all(per, lambda k: ag_mate_copy(k, step))

        gw_out[...] = whole[...]
    q_own.wait()
    wait_all(n, q_copy)


def per_device(n, m, inputs, w_key, w_value, queries, cotangent, cum_gate):
    seq_count, positions, feature_count = inputs.shape
    rows, kv_width = w_key.shape
    kv_heads = kv_width // HD
    query_width = queries.shape[2]
    width = query_width // n
    heads = width // HD
    length = positions * n
    dma = pltpu.SemaphoreType.DMA

    def params(cid):
        return pltpu.CompilerParams(
            collective_id=cid, has_side_effects=True, vmem_limit_bytes=60 * 1024 * 1024
        )

    def shape(dims, dtype=BF16):
        return jax.ShapeDtypeStruct(dims, dtype)

    def blocks(x):
        if width % LANES == 0:
            return x.reshape(positions, query_width)
        return x.reshape(positions, n, width).transpose(1, 0, 2)

    tile = max(256, positions)
    piece = rows // n
    reduce_here = rows % (16 * n) == 0
    gq_shape = (positions, query_width) if width % LANES == 0 else (n, positions, width)
    share_shape = (rows, 2 * kv_width)
    per = n // kv_heads
    out_shape = [
        shape(gq_shape), shape((positions, feature_count)), shape((heads, length), F32)
    ]
    scratch = [
        pltpu.VMEM((length, width), BF16),
        pltpu.VMEM((length, width), BF16),
        pltpu.VMEM((length, 2 * HD), BF16),
        pltpu.VMEM((rows * m, 2 * kv_width), BF16),
        pltpu.VMEM((m, positions, rows), BF16),
        pltpu.VMEM((positions, 2 * kv_width), BF16),
        dma((2, n)), dma((2, n)), dma((2, kv_heads)), dma((kv_heads, 2, per)),
        dma((2, m)), dma((2, m)), dma((2, m)), dma((6,)),
        pltpu.VMEM((heads, length, LANES), BF16),
        pltpu.VMEM((HD, length), BF16),
        pltpu.VMEM((length, HD), BF16),
        pltpu.VMEM((heads, length, LANES), BF16),
        pltpu.VMEM((heads, length, LANES), BF16),
        pltpu.VMEM((heads, length, HD), BF16),
        pltpu.VMEM((heads, length, tile), F32),
        pltpu.VMEM((heads, length, tile), F32),
        pltpu.VMEM((length, LANES), F32),
        pltpu.VMEM((length, HD), F32),
        pltpu.VMEM((length, width), BF16),
        pltpu.VMEM((length, 2 * HD), BF16),
        pltpu.VMEM((per, kv_heads, positions, 2 * HD), BF16),
        pltpu.VMEM((kv_heads, positions, 2 * HD), BF16),
        pltpu.VMEM((kv_heads, positions, 2 * HD), BF16),
        pltpu.VMEM((m, positions, 2 * kv_width), BF16),
        dma((2, n)), dma((kv_heads, 2, per)), dma((2, kv_heads)), dma((2, m)), dma((1,)),
    ]
    if reduce_here:
        out_shape += [shape(share_shape)]
        scratch += [
            pltpu.VMEM(share_shape, BF16),
            pltpu.VMEM((per, kv_heads, piece, 2 * kv_width), BF16),
            pltpu.VMEM((kv_heads, piece, 2 * kv_width), BF16),
            pltpu.VMEM((kv_heads, piece, 2 * kv_width), BF16),
            pltpu.VMEM(share_shape, BF16),
            dma((kv_heads, 2, per)), dma((2, kv_heads)),
            dma((2, kv_heads)), dma((kv_heads, 2, per)),
        ]
    else:
        out_shape += [shape(share_shape)]
    results = pl.pallas_call(
        functools.partial(attend_kernel, n, m, width, kv_heads, tile, reduce_here),
        out_shape=tuple(out_shape),
        in_specs=[VMEM] * 6,
        out_specs=(VMEM,) * len(out_shape),
        scratch_shapes=scratch,
        compiler_params=params(0),
        name="attend_return",
    )(blocks(queries), blocks(cotangent), cum_gate[0], inputs[0], w_key, w_value)
    grad_queries, grad_input, grad_cum = results[:3]
    if width % LANES:
        grad_queries = grad_queries.transpose(1, 0, 2)
    summed = results[3] if reduce_here else lax.psum(results[3], "sp")
    summed = summed.astype(F32)
    grad_wk, grad_wv = summed[:, :kv_width], summed[:, kv_width:]
    return (
        grad_input.reshape(inputs.shape),
        grad_queries.reshape(queries.shape),
        grad_cum.reshape(cum_gate.shape),
        grad_wk,
        grad_wv,
    )


def solution(mesh):
    in_specs = (
        P("dp", "sp", None),
        P("dp", None),
        P("dp", None),
        P("dp", "sp", None),
        P("dp", "sp", None),
        P("dp", "sp", None),
    )
    out_specs = (
        P("dp", "sp", None),
        P("dp", "sp", None),
        P("dp", "sp", None),
        P("dp", None),
        P("dp", None),
    )
    body = functools.partial(per_device, mesh.shape["sp"], mesh.shape["dp"])
    return jax.shard_map(
        body, mesh=mesh, in_specs=in_specs, out_specs=out_specs, check_vma=False
    )
```

```python
import functools

import jax
import jax.numpy as jnp
from jax import lax
from jax.experimental import pallas as pl
from jax.experimental.pallas import tpu as pltpu
from jax.sharding import PartitionSpec as P

HD = 64
LANES = 128
LOG2E = 1.4426950408889634
MESH = pl.DeviceIdType.MESH
VMEM = pl.BlockSpec(memory_space=pltpu.VMEM)
BF16 = jnp.bfloat16
F32 = jnp.float32


def dot_nn(a, b):
    return jnp.dot(a, b, preferred_element_type=F32)


def dot_nt(a, b):
    return lax.dot_general(a, b, (((1,), (1,)), ((), ())), preferred_element_type=F32)


def dot_tn(a, b):
    return lax.dot_general(a, b, (((0,), (0,)), ((), ())), preferred_element_type=F32)


def greet(n, m):
    me, mine = lax.axis_index("sp"), lax.axis_index("dp")
    barrier = pltpu.get_barrier_semaphore()

    @pl.loop(1, n)
    def _(k):
        pl.semaphore_signal(
            barrier, inc=1, device_id={"sp": lax.rem(me + k, n)}, device_id_type=MESH
        )

    @pl.loop(1, m)
    def _(k):
        pl.semaphore_signal(
            barrier, inc=1, device_id={"dp": lax.rem(mine + k, m)}, device_id_type=MESH
        )

    pl.semaphore_wait(barrier, n + m - 2)


def start_all(n, make):
    @pl.loop(1, n)
    def _(k):
        make(k).start()


def wait_all(n, make):
    @pl.loop(1, n)
    def _(k):
        make(k).wait()


def remote(src, dst, sems, k, device):
    return pltpu.make_async_remote_copy(
        src_ref=src,
        dst_ref=dst,
        send_sem=sems.at[0, k],
        recv_sem=sems.at[1, k],
        device_id=device,
        device_id_type=MESH,
    )


def column_block(ref, j, width):
    if len(ref.shape) == 3:
        return ref.at[j]
    return ref.at[:, pl.ds(pl.multiple_of(j * width, LANES), width)]


def row_block(ref, j, rows):
    return ref.at[pl.ds(pl.multiple_of(j * rows, 16), rows)]


def split_bits(gate):
    first = gate.astype(BF16).astype(F32)
    second = (gate - first).astype(BF16).astype(F32)
    third = (gate - first - second).astype(BF16).astype(F32)
    return first, second, third


def attend_kernel(
    n, m, width, kv_heads, tile, reduce_here,
    q_ref, g_ref, gate_ref, x_ref, wk_ref, wv_ref,
    gq_out, gx_out, gc_ref, *rest,
):
    if reduce_here:
        (gw_out, *rest, share, parts, rs_sum, rs_groups, whole,
         rs_mate_sems, rs_sems, ag_sems, ag_mate_sems) = rest
    else:
        share, *rest = rest
    (q_all, g_all, kv_all, w_all, x_all, kv_block,
     qi_sems, g_sems, kvi_sems, matei_sems, wk_sems, wv_sems, x_sems, owni_sems,
     kx, kt, vs, qx, qd, gh, s_buf, d_buf, dk_acc, dv_acc, dq_buf, dkv_buf,
     slots, sums_buf, groups_buf, gkv_all,
     q_sems, mate_sems, group_sems, gkv_sems, own_sems) = rest
    me, mine = lax.axis_index("sp"), lax.axis_index("dp")
    heads = width // HD
    length = kv_all.shape[0]
    positions = x_ref.shape[0]
    rows, kv_width = wk_ref.shape
    per = n // kv_heads
    plane, member = me // per, lax.rem(me, per)
    scale = HD ** (-0.5)
    greet(n, m)

    def target(k):
        return lax.rem(me + k, n)

    def peer(k):
        return lax.rem(mine + k, m)

    def wk_copy(k):
        dst = row_block(w_all, mine, rows).at[:, pl.ds(0, kv_width)]
        return remote(wk_ref, dst, wk_sems, k, {"dp": peer(k)})

    def wv_copy(k):
        dst = row_block(w_all, mine, rows).at[:, pl.ds(kv_width, kv_width)]
        return remote(wv_ref, dst, wv_sems, k, {"dp": peer(k)})

    def x_copy(k):
        return remote(
            column_block(x_ref, peer(k), rows), x_all.at[mine], x_sems, k, {"dp": peer(k)}
        )

    def qi_copy(k):
        return remote(
            column_block(q_ref, target(k), width),
            row_block(q_all, me, positions), qi_sems, k, {"sp": target(k)},
        )

    def g_copy(k):
        return remote(
            column_block(g_ref, target(k), width),
            row_block(g_all, me, positions), g_sems, k, {"sp": target(k)},
        )

    def kvi_copy(k):
        group = lax.rem(plane + k, kv_heads)
        return remote(
            column_block(kv_block, group, 2 * HD),
            row_block(kv_all, me, positions), kvi_sems, k, {"sp": group * per + member},
        )

    def matei_copy(k, step):
        source = lax.rem(plane - step + kv_heads, kv_heads) * per + member
        rows_of = row_block(kv_all, source, positions)
        return remote(
            rows_of, rows_of, matei_sems.at[step], k,
            {"sp": plane * per + lax.rem(member + k, per)},
        )

    own = [
        pltpu.make_async_copy(
            wk_ref, row_block(w_all, mine, rows).at[:, pl.ds(0, kv_width)], owni_sems.at[0]
        ),
        pltpu.make_async_copy(
            wv_ref, row_block(w_all, mine, rows).at[:, pl.ds(kv_width, kv_width)], owni_sems.at[1]
        ),
        pltpu.make_async_copy(column_block(x_ref, mine, rows), x_all.at[mine], owni_sems.at[2]),
        pltpu.make_async_copy(
            column_block(q_ref, me, width), row_block(q_all, me, positions), owni_sems.at[3]
        ),
        pltpu.make_async_copy(
            column_block(g_ref, me, width), row_block(g_all, me, positions), owni_sems.at[4]
        ),
    ]
    start_all(m, wk_copy)
    start_all(m, wv_copy)
    start_all(n, qi_copy)
    for copy in own:
        copy.start()
    wait_all(m, wk_copy)
    wait_all(m, wv_copy)
    for copy in own:
        copy.wait()
    both = dot_nn(x_ref[...], w_all[...]).astype(BF16)
    pieces = []
    for group in range(kv_heads):
        pieces.append(both[:, group * HD : (group + 1) * HD])
        pieces.append(both[:, kv_width + group * HD : kv_width + (group + 1) * HD])
    kv_block[...] = jnp.concatenate(pieces, axis=1)
    start_all(kv_heads, kvi_copy)
    kv_own = pltpu.make_async_copy(
        column_block(kv_block, plane, 2 * HD),
        row_block(kv_all, me, positions), owni_sems.at[5],
    )
    kv_own.start()
    start_all(n, g_copy)
    start_all(m, x_copy)
    kv_own.wait()
    start_all(per, lambda k: matei_copy(k, 0))

    @pl.loop(1, kv_heads)
    def _(step):
        kvi_copy(step).wait()
        start_all(per, lambda k: matei_copy(k, step))

    def q_copy(k):
        return remote(
            row_block(dq_buf, target(k), positions),
            column_block(gq_out, me, width), q_sems, k, {"sp": target(k)},
        )

    def mate_copy(k, a):
        to = lax.rem(member + k, per)
        return remote(
            row_block(dkv_buf, a * per + to, positions), slots.at[member, a],
            mate_sems.at[a], k, {"sp": plane * per + to},
        )

    def group_copy(k):
        a = lax.rem(plane + k, kv_heads)
        return remote(
            sums_buf.at[a], groups_buf.at[plane], group_sems, k, {"sp": a * per + member}
        )

    def gkv_copy(k):
        return remote(gkv_all.at[mine], gkv_all.at[mine], gkv_sems, k, {"dp": peer(k)})

    q_own = pltpu.make_async_copy(
        row_block(dq_buf, me, positions), column_block(gq_out, me, width), own_sems.at[0]
    )

    def send_tile(i):
        for part in range(tile // positions):
            j = i * (tile // positions) + part
            k = lax.rem(j - me + n, n)
            a, b = j // per, lax.rem(j, per)
            km = lax.rem(b - member + per, per)

            @pl.when(km != 0)
            def _():
                mate_copy(km, a).start()

            @pl.when(k != 0)
            def _():
                q_copy(k).start()

    lane = lax.broadcasted_iota(jnp.int32, (length, HD), 1)
    ones = jnp.ones((3, length), F32)
    blank = jnp.zeros((HD - 6, length), F32)
    dk_acc[...] = jnp.zeros_like(dk_acc)
    dv_acc[...] = jnp.zeros_like(dv_acc)
    wait_all(n, qi_copy)
    for h in range(heads):
        three = jnp.concatenate(split_bits(gate_ref[h : h + 1, :]), axis=0)
        gates = jnp.concatenate([ones, three, blank, -three, ones, blank], axis=0).T.astype(BF16)
        q_head = q_all[:, h * HD : (h + 1) * HD]
        kx[h, :, HD:] = gates[:, HD:]
        qx[h] = jnp.concatenate([q_head * jnp.asarray(scale, BF16), gates[:, :HD]], axis=1)
        mark = jnp.where(lane == h, 1.0, 0.0).astype(BF16)
        qd[h] = jnp.concatenate([q_head, mark], axis=1)
    wait_all(n, g_copy)
    for h in range(heads):
        gh[h] = g_all[:, h * HD : (h + 1) * HD]

    @pl.loop(0, kv_heads)
    def _(step):
        wait_all(per, lambda k: matei_copy(k, step))

    wait_all(m, x_copy)
    keys = kv_all[:, :HD]
    kt[...] = keys.astype(F32).T.astype(BF16)
    vs[...] = kv_all[:, HD:]
    for h in range(heads):
        kx[h, :, :HD] = keys
    later = lax.broadcasted_iota(jnp.int32, (tile, tile), 0) > lax.broadcasted_iota(
        jnp.int32, (tile, tile), 1
    )
    every = range(heads)

    def fold(op, a):
        return op(a.reshape(tile // 8, 8, tile), axis=0)

    tiles = length // tile

    @pl.loop(0, tiles)
    def _(turn):
        i = tiles - 1 - turn
        here = pl.ds(pl.multiple_of(i * tile, tile), tile)

        def score(c, tops, diagonal):
            at = pl.ds(pl.multiple_of(c * tile, tile), tile)
            out = []
            for h in every:
                s = dot_nt(kx[h, at, :], qx[h, here, :])
                if diagonal:
                    s = jnp.where(later, -jnp.inf, s)
                s_buf[h, at, :] = s
                out.append(jnp.maximum(tops[h], fold(jnp.max, s)))
            return tuple(out)

        tops = tuple(jnp.full((8, tile), -jnp.inf, F32) for _ in every)
        tops = lax.fori_loop(0, i, lambda c, v: score(c, v, False), tops)
        tops = score(i, tops, True)

        @pl.when(turn > 0)
        def _():
            send_tile(i + 1)

        tops = [jnp.max(top, axis=0, keepdims=True) for top in tops]

        def weigh(c, carry):
            at = pl.ds(pl.multiple_of(c * tile, tile), tile)
            out = []
            for h in every:
                total, dots = carry[h]
                d = dot_nt(vs[at, :], gh[h, here, :])
                e = jnp.exp2((s_buf[h, at, :] - tops[h]) * LOG2E)
                s_buf[h, at, :] = e
                d_buf[h, at, :] = d
                out.append((total + fold(jnp.sum, e), dots + fold(jnp.sum, e * d)))
            return tuple(out)

        zero = jnp.zeros((8, tile), F32)
        sums = lax.fori_loop(0, i + 1, weigh, tuple((zero, zero) for _ in every))
        inverse, row_dot = [], []
        for h in every:
            total = jnp.sum(sums[h][0], axis=0, keepdims=True)
            dots = jnp.sum(sums[h][1], axis=0, keepdims=True)
            inv = 1.0 / total
            inverse.append(inv)
            row_dot.append(dots * inv)
            gc_ref[h : h + 1, here] = dots * inv - row_dot[h] * (total * inv)

        def spread(c, carry):
            at = pl.ds(pl.multiple_of(c * tile, tile), tile)
            out = []
            dk = dk_acc[at, :]
            dv = dv_acc[at, :]
            for h in every:
                p = s_buf[h, at, :] * inverse[h]
                low = (p * (d_buf[h, at, :] - row_dot[h])).astype(BF16)
                dv = dv + dot_nn(p.astype(BF16), gh[h, here, :])
                dk = dk + dot_nn(low, qd[h, here, :])
                out.append(carry[h] + dot_nn(kt[:, at], low))
            dk_acc[at, :] = dk
            dv_acc[at, :] = dv
            return tuple(out)

        start = tuple(jnp.zeros((HD, tile), F32) for _ in every)
        grads = lax.fori_loop(0, i + 1, spread, start)
        dq_buf[here, :] = jnp.concatenate([gr.T * scale for gr in grads], axis=1).astype(BF16)
        dkv_buf[here, :] = jnp.concatenate(
            [dk_acc[here, :][:, :HD] * scale, dv_acc[here, :]], axis=1
        ).astype(BF16)

    send_tile(0)
    q_own.start()
    columns = dk_acc[...].T
    gc_ref[...] = gc_ref[...] - columns[HD : HD + heads, :]

    @pl.loop(0, kv_heads)
    def _(step):
        a = lax.rem(plane + 1 + step, kv_heads)
        wait_all(per, lambda k: mate_copy(k, a))
        rows_of = row_block(dkv_buf, a * per + member, positions)
        total = rows_of[...].astype(F32)
        for k in range(1, per):
            total = total + slots[lax.rem(member + k, per), a].astype(F32)
        sums_buf[a] = total.astype(BF16)

        @pl.when(step < kv_heads - 1)
        def _():
            group_copy(step + 1).start()

    groups_buf[plane] = sums_buf[plane]
    wait_all(kv_heads, group_copy)
    groups = [groups_buf[group] for group in range(kv_heads)]
    gkv = jnp.concatenate(
        [total[:, :HD] for total in groups] + [total[:, HD:] for total in groups], axis=1
    )
    gkv_all[mine] = gkv
    start_all(m, gkv_copy)
    gx_out[...] = dot_nt(gkv, w_all[...]).astype(BF16)
    wait_all(m, gkv_copy)
    total = dot_tn(x_all[0], gkv_all[0])
    for j in range(1, m):
        total = total + dot_tn(x_all[j], gkv_all[j])
    share[...] = total.astype(BF16)
    if reduce_here:
        piece = rows // n

        def rs_mate_copy(k, a):
            to = lax.rem(member + k, per)
            return remote(
                row_block(share, a * per + to, piece), parts.at[member, a],
                rs_mate_sems.at[a], k, {"sp": plane * per + to},
            )

        def rs_copy(k):
            a = lax.rem(plane + k, kv_heads)
            return remote(
                rs_sum.at[a], rs_groups.at[plane], rs_sems, k, {"sp": a * per + member}
            )

        def ag_copy(k):
            block = row_block(whole, me, piece)
            to = lax.rem(plane + k, kv_heads) * per + member
            return remote(block, block, ag_sems, k, {"sp": to})

        def ag_mate_copy(k, step):
            source = lax.rem(plane - step + kv_heads, kv_heads) * per + member
            block = row_block(whole, source, piece)
            to = plane * per + lax.rem(member + k, per)
            return remote(block, block, ag_mate_sems.at[step], k, {"sp": to})

        @pl.loop(0, kv_heads)
        def _(step):
            start_all(per, lambda k: rs_mate_copy(k, lax.rem(plane + 1 + step, kv_heads)))

        @pl.loop(0, kv_heads)
        def _(step):
            a = lax.rem(plane + 1 + step, kv_heads)
            wait_all(per, lambda k: rs_mate_copy(k, a))
            total = row_block(share, a * per + member, piece)[...].astype(F32)
            for k in range(1, per):
                total = total + parts[lax.rem(member + k, per), a].astype(F32)
            rs_sum[a] = total.astype(BF16)

            @pl.when(step < kv_heads - 1)
            def _():
                rs_copy(step + 1).start()

        total = rs_sum[plane].astype(F32)
        for k in range(1, kv_heads):
            rs_copy(k).wait()
            total = total + rs_groups[lax.rem(plane - k + kv_heads, kv_heads)].astype(F32)
        row_block(whole, me, piece)[...] = total.astype(BF16)
        start_all(kv_heads, ag_copy)
        start_all(per, lambda k: ag_mate_copy(k, 0))

        @pl.loop(1, kv_heads)
        def _(step):
            ag_copy(step).wait()
            start_all(per, lambda k: ag_mate_copy(k, step))

        @pl.loop(0, kv_heads)
        def _(step):
            wait_all(per, lambda k: ag_mate_copy(k, step))

        gw_out[...] = whole[...]
    q_own.wait()
    wait_all(n, q_copy)


def per_device(n, m, inputs, w_key, w_value, queries, cotangent, cum_gate):
    seq_count, positions, feature_count = inputs.shape
    rows, kv_width = w_key.shape
    kv_heads = kv_width // HD
    query_width = queries.shape[2]
    width = query_width // n
    heads = width // HD
    length = positions * n
    dma = pltpu.SemaphoreType.DMA

    def params(cid):
        return pltpu.CompilerParams(
            collective_id=cid, has_side_effects=True, vmem_limit_bytes=60 * 1024 * 1024
        )

    def shape(dims, dtype=BF16):
        return jax.ShapeDtypeStruct(dims, dtype)

    def blocks(x):
        if width % LANES == 0:
            return x.reshape(positions, query_width)
        return x.reshape(positions, n, width).transpose(1, 0, 2)

    tile = max(512, positions)
    piece = rows // n
    reduce_here = rows % (16 * n) == 0
    gq_shape = (positions, query_width) if width % LANES == 0 else (n, positions, width)
    share_shape = (rows, 2 * kv_width)
    per = n // kv_heads
    out_shape = [
        shape(gq_shape), shape((positions, feature_count)), shape((heads, length), F32)
    ]
    scratch = [
        pltpu.VMEM((length, width), BF16),
        pltpu.VMEM((length, width), BF16),
        pltpu.VMEM((length, 2 * HD), BF16),
        pltpu.VMEM((rows * m, 2 * kv_width), BF16),
        pltpu.VMEM((m, positions, rows), BF16),
        pltpu.VMEM((positions, 2 * kv_width), BF16),
        dma((2, n)), dma((2, n)), dma((2, kv_heads)), dma((kv_heads, 2, per)),
        dma((2, m)), dma((2, m)), dma((2, m)), dma((6,)),
        pltpu.VMEM((heads, length, LANES), BF16),
        pltpu.VMEM((HD, length), BF16),
        pltpu.VMEM((length, HD), BF16),
        pltpu.VMEM((heads, length, LANES), BF16),
        pltpu.VMEM((heads, length, LANES), BF16),
        pltpu.VMEM((heads, length, HD), BF16),
        pltpu.VMEM((heads, length, tile), F32),
        pltpu.VMEM((heads, length, tile), F32),
        pltpu.VMEM((length, LANES), F32),
        pltpu.VMEM((length, HD), F32),
        pltpu.VMEM((length, width), BF16),
        pltpu.VMEM((length, 2 * HD), BF16),
        pltpu.VMEM((per, kv_heads, positions, 2 * HD), BF16),
        pltpu.VMEM((kv_heads, positions, 2 * HD), BF16),
        pltpu.VMEM((kv_heads, positions, 2 * HD), BF16),
        pltpu.VMEM((m, positions, 2 * kv_width), BF16),
        dma((2, n)), dma((kv_heads, 2, per)), dma((2, kv_heads)), dma((2, m)), dma((1,)),
    ]
    if reduce_here:
        out_shape += [shape(share_shape)]
        scratch += [
            pltpu.VMEM(share_shape, BF16),
            pltpu.VMEM((per, kv_heads, piece, 2 * kv_width), BF16),
            pltpu.VMEM((kv_heads, piece, 2 * kv_width), BF16),
            pltpu.VMEM((kv_heads, piece, 2 * kv_width), BF16),
            pltpu.VMEM(share_shape, BF16),
            dma((kv_heads, 2, per)), dma((2, kv_heads)),
            dma((2, kv_heads)), dma((kv_heads, 2, per)),
        ]
    else:
        out_shape += [shape(share_shape)]
    results = pl.pallas_call(
        functools.partial(attend_kernel, n, m, width, kv_heads, tile, reduce_here),
        out_shape=tuple(out_shape),
        in_specs=[VMEM] * 6,
        out_specs=(VMEM,) * len(out_shape),
        scratch_shapes=scratch,
        compiler_params=params(0),
        name="attend_return",
    )(blocks(queries), blocks(cotangent), cum_gate[0], inputs[0], w_key, w_value)
    grad_queries, grad_input, grad_cum = results[:3]
    if width % LANES:
        grad_queries = grad_queries.transpose(1, 0, 2)
    summed = results[3] if reduce_here else lax.psum(results[3], "sp")
    summed = summed.astype(F32)
    grad_wk, grad_wv = summed[:, :kv_width], summed[:, kv_width:]
    return (
        grad_input.reshape(inputs.shape),
        grad_queries.reshape(queries.shape),
        grad_cum.reshape(cum_gate.shape),
        grad_wk,
        grad_wv,
    )


def solution(mesh):
    in_specs = (
        P("dp", "sp", None),
        P("dp", None),
        P("dp", None),
        P("dp", "sp", None),
        P("dp", "sp", None),
        P("dp", "sp", None),
    )
    out_specs = (
        P("dp", "sp", None),
        P("dp", "sp", None),
        P("dp", "sp", None),
        P("dp", None),
        P("dp", None),
    )
    body = functools.partial(per_device, mesh.shape["sp"], mesh.shape["dp"])
    return jax.shard_map(
        body, mesh=mesh, in_specs=in_specs, out_specs=out_specs, check_vma=False
    )
```
